32 devices in a mesh: kv: 4 (over y, x), tp: 8 (over z, core).
Axes of the slice: x: 2, y: 2, z: 4, core: 2. Of those that a mesh axis runs over, the one named last changes fastest.
Arguments:
- stream: bfloat16 [32, 4096], P(None, ('kv', 'tp')), may hold values from -18 to 18
- mixer_gain: float32 [4096], replicated, may hold values from 0.1 to 1.9
- query_weight: bfloat16 [4096, 1024], P(None, 'tp'), may hold values from -0.09375 to 0.09375
- key_weight: bfloat16 [4096, 1024], P(None, 'tp'), may hold values from -0.09375 to 0.09375
- value_weight: bfloat16 [4096, 1024], P(None, 'tp'), may hold values from -0.09375 to 0.09375
- forget_weight: bfloat16 [4096, 16], replicated, may hold values from -0.09375 to 0.09375
- forget_bias: float32 [16], replicated, may hold values from -4 to -2
- key_cache: bfloat16 [32, 16, 4096, 64], P(None, 'tp', 'kv'), may hold values from -512 to 512, as said below
- value_cache: bfloat16 [32, 16, 4096, 64], P(None, 'tp', 'kv'), may hold values from -12 to 12
- past_decay: float32 [32, 16, 4096], P(None, 'tp', 'kv'), may hold values from -4096 to 0, as said below
- out_weight: bfloat16 [1024, 4096], P('tp', 'kv'), may hold values from -0.75 to 0.75
- channel_gain: float32 [4096], replicated, may hold values from 0.1 to 1.9
- up_weight: bfloat16 [4096, 16384], P('kv', 'tp'), may hold values from -0.09375 to 0.09375
- down_weight: bfloat16 [16384, 4096], P('tp', 'kv'), may hold values from -0.0625 to 0.0625
Outputs:
- updated: bfloat16 [32, 4096], P(None, ('kv', 'tp'))
The draws below stay inside these ranges and needn't reach their ends.
Inputs may be any that keep to these rules, and one draw needn't show every extreme that they name: `key_cache`: keys of order one; some cached keys may be much larger. `past_decay`: never falling along the positions of a sequence and head, zero at the last cached position.
All inputs are finite; a program needn't handle non-finite values.
Results may differ from the reference program's by a relative error of at most 0.014.
The reference program's roundings to bfloat16 on the way count: a program that leaves them out, or rounds other values in their place, can miss the bound.
Values may be sent and summed in bfloat16 or wider, within the bound.
No kernel may reach another device: no remote copies, remote signals or barrier semaphores. Data moves between devices by JAX's collectives and lax.ppermute only.
A program may use at most 64 MiB of HBM per device.

```python
import math
import jax
import jax.numpy as jnp
from jax import lax

D = 4096
HEADS = 16
HEAD = 64
FF = 16384
BATCH = 32
POS_DEV = 1024
BLOCK = 256
CACHE = 4096


def draw_stream(key, part):
    first_key = jax.random.fold_in(jax.random.fold_in(key, 5), 0)
    columns = jnp.exp(jnp.linspace(0.0, math.log(3.0), D).astype(jnp.float32))
    base = jax.random.normal(first_key, (BATCH, D), jnp.float32)
    values = jnp.clip(base, -6.0, 6.0) * columns[None, :]
    return values.astype(jnp.bfloat16)


def draw_key_cache(key, part):
    first_key = jax.random.fold_in(jax.random.fold_in(key, 11), 0)
    values = 2.0 * jax.random.normal(first_key, (BATCH, HEADS, CACHE, HEAD), jnp.float32)
    values = jnp.clip(values, -12.0, 12.0)
    return values.astype(jnp.bfloat16)


def draw_value_cache(key, part):
    first_key, offset_key = jax.random.split(jax.random.fold_in(key, 23), 2)
    base = jax.random.normal(first_key, (BATCH, HEADS, CACHE, HEAD), jnp.float32)
    offsets = jax.random.normal(offset_key, (BATCH, HEADS, CACHE // BLOCK, 1, HEAD), jnp.float32)
    offsets = jnp.broadcast_to(offsets, (BATCH, HEADS, CACHE // BLOCK, BLOCK, HEAD)).reshape(BATCH, HEADS, CACHE, HEAD)
    return jnp.clip(base + offsets, -12.0, 12.0).astype(jnp.bfloat16)


def draw_past_decay(key, part):
    pick_key, rate_key, block_key, rough_key = jax.random.split(jax.random.fold_in(key, 37), 4)
    fast = jax.random.uniform(pick_key, (1, HEADS, 1)) < 0.5
    fast_rate = jnp.exp(jax.random.uniform(rate_key, (1, HEADS, 1), jnp.float32, math.log(1.0 / 30.0), math.log(1.0 / 12.0)))
    rate = jnp.where(fast, fast_rate, 0.5 / CACHE)
    block_factor = jnp.exp(jax.random.uniform(block_key, (BATCH, HEADS, CACHE // BLOCK, 1), jnp.float32, -math.log(4.0), math.log(4.0)))
    block_factor = jnp.broadcast_to(block_factor, (BATCH, HEADS, CACHE // BLOCK, BLOCK)).reshape(BATCH, HEADS, CACHE)
    rough = jnp.exp(jax.random.uniform(rough_key, (BATCH, HEADS, CACHE), jnp.float32, -math.log(2.0), math.log(2.0)))
    log_gates = -rate * block_factor * rough
    after = jnp.flip(jnp.cumsum(jnp.flip(log_gates, -1), -1), -1) - log_gates
    return jnp.clip(after, -1.0 * CACHE, 0.0)


def strengthened(values, rng, source, target, parts, factor):
    owner, partner = [(jnp.arange(values.shape[position]) // (values.shape[position] // parts)).reshape([-1 if axis == position else 1 for axis in range(values.ndim)]) for position in (source, target)]
    chosen = jax.random.permutation(rng, parts)[partner]
    strong = (owner == chosen) | (owner == (partner + parts // 2) % parts)
    return jnp.where(strong, factor * values, values)


def block_levels(stream_key, dims, shards, least, high):
    def one(dim, parts):
        heights = jax.random.uniform(jax.random.fold_in(jax.random.fold_in(stream_key, 6), dim), (parts,), jnp.float32, least / len(shards), high / len(shards))
        return jnp.repeat(jnp.exp(heights), dims[dim] // parts).reshape((-1,) + (1,) * (len(dims) - dim - 1))

    level = one(*shards[0])
    for cut in shards[1:]:
        level = level * one(*cut)
    return level


def normal_values(rng, dims, deviation, reach, cuts=(), held_as=jnp.bfloat16):
    array = deviation * jax.random.normal(rng, dims, jnp.float32)
    if cuts:
        array = array * block_levels(rng, dims, cuts, -0.22, 0.18)
    return jnp.clip(array, -reach, reach).astype(held_as)


def noise_with(rng, dims, deviation, bound, cuts, heavy, held_as=jnp.bfloat16):
    entries = deviation * jax.random.normal(rng, dims, jnp.float32)
    if cuts:
        entries = entries * block_levels(rng, dims, cuts, -0.22, 0.18)
    return jnp.clip(strengthened(entries, jax.random.fold_in(rng, 3), *heavy), -bound, bound).astype(held_as)


def setup_inputs(seed: int = 0) -> dict:
    streams_of = jax.random.split(jax.random.key(seed), 15)
    return {
        "stream": draw_stream(jax.random.fold_in(streams_of[14], 71), 0),
        "mixer_gain": jnp.clip(1.0 + 0.18 * jax.random.normal(streams_of[1], (D,), jnp.float32), 0.1, 1.9),
        "query_weight": normal_values(streams_of[2], (D, HEADS * HEAD), D ** -0.5, 0.09375, ((1, 8),)),
        "key_weight": normal_values(streams_of[3], (D, HEADS * HEAD), D ** -0.5, 0.09375, ((1, 8),)),
        "value_weight": normal_values(streams_of[4], (D, HEADS * HEAD), D ** -0.5, 0.09375, ((1, 8),)),
        "forget_weight": normal_values(streams_of[5], (D, HEADS), D ** -0.5, 0.09375),
        "forget_bias": jnp.clip(jax.random.uniform(streams_of[6], (HEADS,), jnp.float32, -4.0, -2.0), -4.0, -2.0),
        "key_cache": draw_key_cache(jax.random.fold_in(streams_of[14], 71), 0),
        "value_cache": draw_value_cache(jax.random.fold_in(streams_of[14], 71), 0),
        "past_decay": draw_past_decay(jax.random.fold_in(streams_of[14], 71), 0),
        "out_weight": noise_with(streams_of[10], (HEADS * HEAD, D), (HEADS * HEAD // 8) ** -0.5, 0.75, ((0, 8), (1, 4)), (0, 1, 8, 2.0)),
        "channel_gain": jnp.clip(1.0 + 0.18 * jax.random.normal(streams_of[11], (D,), jnp.float32), 0.1, 1.9),
        "up_weight": normal_values(streams_of[12], (D, FF), D ** -0.5, 0.09375, ((0, 4), (1, 8))),
        "down_weight": noise_with(streams_of[13], (FF, D), FF ** -0.5, 0.0625, ((0, 8), (1, 4)), (0, 1, 8, 2.0)),
    }


EPS = 1e-06

def rms_scale(values, gain):
    widened = values.astype(jnp.float32)
    inverse = lax.rsqrt(lax.optimization_barrier(jnp.mean(widened * widened, axis=-1, keepdims=True)) + EPS)
    return (widened * inverse * gain.astype(jnp.float32)).astype(jnp.bfloat16)

def reference(stream, mixer_gain, query_weight, key_weight, value_weight, forget_weight, forget_bias, key_cache, value_cache, past_decay, out_weight, channel_gain, up_weight, down_weight):
    scale_factor = float(HEAD) ** (-0.5)
    normed = rms_scale(stream, mixer_gain)
    queries = jnp.dot(normed, query_weight, preferred_element_type=jnp.float32).astype(jnp.bfloat16)
    keys_new = jnp.dot(normed, key_weight, preferred_element_type=jnp.float32).astype(jnp.bfloat16)
    values_new = jnp.dot(normed, value_weight, preferred_element_type=jnp.float32).astype(jnp.bfloat16)
    forget = jax.nn.log_sigmoid(jnp.dot(normed, forget_weight, preferred_element_type=jnp.float32) + forget_bias.astype(jnp.float32))
    query_heads = queries.reshape(BATCH, HEADS, HEAD).astype(jnp.float32)
    key_heads = keys_new.reshape(BATCH, HEADS, HEAD).astype(jnp.float32)
    value_heads = values_new.reshape(BATCH, HEADS, HEAD).astype(jnp.float32)
    block_count = CACHE // POS_DEV

    def per_head(index):
        keys = lax.dynamic_index_in_dim(key_cache, index, 1, keepdims=False).astype(jnp.float32)
        values = lax.dynamic_index_in_dim(value_cache, index, 1, keepdims=False).astype(jnp.float32)
        decay = lax.dynamic_index_in_dim(past_decay, index, 1, keepdims=False).astype(jnp.float32)
        query_one = lax.dynamic_index_in_dim(query_heads, index, 1, keepdims=False)
        forget_one = lax.dynamic_index_in_dim(forget, index, 1, keepdims=False)
        scores = jnp.einsum('bd,bpd->bp', query_one, keys) * scale_factor + forget_one[:, None] + decay
        scores = scores.reshape(BATCH, block_count, POS_DEV)
        tops = lax.optimization_barrier(jnp.max(scores, axis=-1))
        weights = jnp.exp(scores - tops[..., None]).astype(jnp.bfloat16)
        weights = lax.optimization_barrier(weights).astype(jnp.float32)
        totals = lax.optimization_barrier(jnp.sum(weights, axis=-1))
        sums = jnp.einsum('bnp,bnpd->bnd', weights, values.reshape(BATCH, block_count, POS_DEV, HEAD))
        return (tops, totals, sums)
    tops, totals, sums = lax.map(per_head, jnp.arange(HEADS).astype(jnp.int32))
    own = (lax.optimization_barrier(jnp.sum(query_heads * key_heads, axis=-1)) * scale_factor).T
    peak = jnp.maximum(lax.optimization_barrier(jnp.max(tops, axis=-1)), own)
    factors = jnp.exp(tops - peak[..., None])
    own_factor = jnp.exp(own - peak)
    numer = lax.optimization_barrier(jnp.sum(sums * factors[..., None], axis=2)) + jnp.transpose(value_heads, (1, 0, 2)) * own_factor[..., None]
    denom = lax.optimization_barrier(jnp.sum(totals * factors, axis=-1)) + own_factor
    attention = jnp.transpose(numer / denom[..., None], (1, 0, 2)).reshape(BATCH, HEADS * HEAD).astype(jnp.bfloat16)
    middle = (stream.astype(jnp.float32) + jnp.dot(attention, out_weight, preferred_element_type=jnp.float32)).astype(jnp.bfloat16)
    mixed = rms_scale(middle, channel_gain)
    hidden = jnp.square(jax.nn.relu(jnp.dot(mixed, up_weight, preferred_element_type=jnp.float32))).astype(jnp.bfloat16)
    return (middle.astype(jnp.float32) + jnp.dot(hidden, down_weight, preferred_element_type=jnp.float32)).astype(jnp.bfloat16)
```

```python
import functools

import jax
import jax.numpy as jnp
from jax import lax
from jax.experimental import pallas as pl
from jax.experimental.pallas import tpu as pltpu
from jax.sharding import PartitionSpec as P

D = 4096


EPS = 1e-06


def combined_all(part, axis, combine):
    gathered = jax.tree.map(lambda a: lax.all_gather(a, axis), part)

    def take(source):
        return jax.tree.map(lambda a: lax.dynamic_index_in_dim(a, source, 0, False), gathered)

    return lax.fori_loop(
        1, lax.axis_size(axis), lambda source, state: combine(state, take(source)), take(0)
    )


def rms_scale(values, gain):
    widened = values.astype(jnp.float32)
    inverse = lax.rsqrt(jnp.mean(widened * widened, axis=-1, keepdims=True) + EPS)
    return (widened * inverse * gain).astype(jnp.bfloat16)


def merge_parts(earlier, later):
    top_one, total_one, sums_one = earlier
    top_two, total_two, sums_two = later
    highest = jnp.maximum(top_one, top_two)
    factor_one = jnp.exp(top_one - highest)
    factor_two = jnp.exp(top_two - highest)
    return (
        highest,
        total_one * factor_one + total_two * factor_two,
        sums_one * factor_one[..., None] + sums_two * factor_two[..., None],
    )


def squared_relu(values):
    return jnp.square(jax.nn.relu(values)).astype(jnp.bfloat16)


def row_squares(values):
    widened = values.astype(jnp.float32)
    return jnp.sum(widened * widened, axis=1)


def shards_general(
    stream,
    mixer_gain,
    query_weight,
    key_weight,
    value_weight,
    forget_weight,
    forget_bias,
    key_cache,
    value_cache,
    past_decay,
    out_weight,
    channel_gain,
    up_weight,
    down_weight,
):
    batch_rows = stream.shape[0]
    local_heads = key_cache.shape[1]
    head_size = key_cache.shape[3]
    scale_factor = float(head_size) ** (-0.5)
    gathered = lax.all_gather(stream, ("kv", "tp"), axis=1, tiled=True)
    normed = rms_scale(gathered, mixer_gain)
    queries = jnp.dot(normed, query_weight, preferred_element_type=jnp.float32).astype(jnp.bfloat16)
    keys_new = jnp.dot(normed, key_weight, preferred_element_type=jnp.float32).astype(jnp.bfloat16)
    values_new = jnp.dot(normed, value_weight, preferred_element_type=jnp.float32).astype(
        jnp.bfloat16
    )
    forget_all = jax.nn.log_sigmoid(
        jnp.dot(normed, forget_weight, preferred_element_type=jnp.float32) + forget_bias
    )
    forget = lax.dynamic_slice_in_dim(
        forget_all, lax.axis_index("tp") * local_heads, local_heads, 1
    )
    query_heads = queries.reshape(batch_rows, local_heads, head_size)
    scores = (
        jnp.einsum("bhd,bhpd->bhp", query_heads, key_cache, preferred_element_type=jnp.float32)
        * scale_factor
        + forget[..., None]
        + past_decay
    )
    highest = jnp.max(scores, axis=-1)
    weights = jnp.exp(scores - highest[..., None]).astype(jnp.bfloat16)
    totals = jnp.sum(weights.astype(jnp.float32), axis=-1)
    sums = jnp.einsum("bhp,bhpd->bhd", weights, value_cache, preferred_element_type=jnp.float32)
    highest, totals, sums = combined_all((highest, totals, sums), "kv", merge_parts)
    key_heads = keys_new.reshape(batch_rows, local_heads, head_size).astype(jnp.float32)
    value_heads = values_new.reshape(batch_rows, local_heads, head_size).astype(jnp.float32)
    own = jnp.sum(query_heads.astype(jnp.float32) * key_heads, axis=-1) * scale_factor
    peak = jnp.maximum(highest, own)
    cache_factor = jnp.exp(highest - peak)
    own_factor = jnp.exp(own - peak)
    numer = sums * cache_factor[..., None] + value_heads * own_factor[..., None]
    denom = totals * cache_factor + own_factor
    attention = (
        (numer / denom[..., None]).astype(jnp.bfloat16).reshape(batch_rows, local_heads * head_size)
    )
    partial_value = jnp.dot(attention, out_weight, preferred_element_type=jnp.float32)
    piece_width = stream.shape[1]
    block_width = partial_value.shape[1]
    block_sum = lax.psum(partial_value, "tp")
    own_block = lax.dynamic_slice_in_dim(
        gathered, lax.axis_index("kv") * block_width, block_width, 1
    )
    middle_block = (own_block.astype(jnp.float32) + block_sum).astype(jnp.bfloat16)
    squares = lax.psum(row_squares(middle_block), "kv")
    middle_piece = lax.dynamic_slice_in_dim(
        middle_block, lax.axis_index("tp") * piece_width, piece_width, 1
    )
    inverse = lax.rsqrt(squares / D + EPS)
    gain_block = lax.dynamic_slice_in_dim(
        channel_gain, lax.axis_index("kv") * block_width, block_width, 0
    )
    mixed_block = (
        middle_block.astype(jnp.float32) * inverse[:, None] * gain_block[None, :]
    ).astype(jnp.bfloat16)
    up_partial = jnp.dot(mixed_block, up_weight, preferred_element_type=jnp.float32)
    hidden = squared_relu(lax.psum(up_partial, "kv"))
    down_partial = jnp.dot(hidden, down_weight, preferred_element_type=jnp.float32)
    reduced = lax.psum_scatter(down_partial, "tp", scatter_dimension=1, tiled=True)
    return (middle_piece.astype(jnp.float32) + reduced).astype(jnp.bfloat16)


LANES = 128
HEAD_LANES = 64
F32 = jnp.float32
BF16 = jnp.bfloat16
CONTRACT_LAST = (((1,), (1,)), ((), ()))


def iota(shape, axis):
    return lax.broadcasted_iota(jnp.int32, shape, axis)


def dot(one, two):
    return jnp.dot(one, two, preferred_element_type=F32)


def exact_dot(one, two):
    return jnp.dot(one, two, preferred_element_type=F32, precision=lax.Precision.HIGHEST)


def kernel_call(body, out_shapes, arguments, scratch=(), limit=8, cost=None):
    return pl.pallas_call(
        body,
        out_shape=tuple(out_shapes),
        in_specs=[pl.BlockSpec(memory_space=pltpu.VMEM)] * len(arguments),
        out_specs=tuple(pl.BlockSpec(memory_space=pltpu.VMEM) for _ in out_shapes),
        scratch_shapes=list(scratch),
        cost_estimate=cost,
        compiler_params=pltpu.CompilerParams(vmem_limit_bytes=limit << 20),
    )(*arguments)


def shape_of(shape, dtype):
    return jax.ShapeDtypeStruct(shape, dtype)


def fan_kernel(piece, copies):
    value = piece[...]
    for index in range(copies.shape[0]):
        copies[index] = value


def attention_kernel(
    local_heads,
    blocks,
    gain,
    query_weight,
    key_weight,
    value_weight,
    forget_weight,
    forget_bias,
    keys,
    values,
    decay,
    part,
    newest,
    normed,
):
    groups = keys.shape[0]
    count, batch, _ = blocks.shape
    rows = batch * local_heads
    squares = jnp.zeros((batch, LANES), F32)
    for block in range(count):
        wide = blocks[block].astype(F32)
        squares = squares + wide * wide
    mean = jnp.sum(squares, axis=1, keepdims=True) / (count * LANES)
    inverse = lax.rsqrt(mean + EPS)
    for block in range(count):
        scaled = blocks[block].astype(F32) * inverse * gain[block : block + 1, :]
        normed[:, block * LANES : (block + 1) * LANES] = scaled.astype(BF16)
    rounded = normed[...]
    query = dot(rounded, query_weight[...]).astype(BF16)
    logits = lax.dot_general(
        rounded, forget_weight[...], CONTRACT_LAST, preferred_element_type=F32
    )
    logits = logits + forget_bias[...]
    forget = jnp.minimum(logits, 0.0) - jnp.log1p(jnp.exp(-jnp.abs(logits)))
    spread = (iota((rows, batch), 0) // local_heads == iota((rows, batch), 1)).astype(F32)
    head_of_row = iota((rows, 1), 0) % local_heads
    heads = forget.shape[1]
    own_head = iota((rows, heads), 1) == lax.axis_index("tp") * local_heads + head_of_row
    forget_rows = jnp.sum(
        jnp.where(own_head, exact_dot(spread, forget), 0.0), axis=1, keepdims=True
    )
    spread_short = spread.astype(BF16)
    query_rows = dot(spread_short, query)
    depth = keys.shape[1]
    per_group = rows // groups
    repeats = depth // query_rows.shape[1]
    query_wide = jnp.concatenate([query_rows] * repeats, axis=1)
    diagonal = iota((rows, depth), 1) // HEAD_LANES == iota((rows, depth), 0) % per_group
    query_wide = jnp.where(diagonal, query_wide, 0.0).astype(BF16)
    diagonal = iota((per_group, depth), 1) // HEAD_LANES == iota((per_group, depth), 0)
    lane = iota((per_group, LANES), 1)
    scale = float(HEAD_LANES) ** (-0.5)
    batches = batch // groups
    for group in range(groups):
        low = group * per_group
        scores = dot(query_wide[low : low + per_group], keys[group]) * scale
        fade = decay[group * batches : (group + 1) * batches].reshape(per_group, -1)
        scores = scores + forget_rows[low : low + per_group] + fade
        top = jnp.max(scores, axis=1, keepdims=True)
        weights = jnp.exp(scores - top).astype(BF16)
        total = jnp.sum(weights.astype(F32), axis=1, keepdims=True)
        sums = lax.dot_general(
            weights, values[group], CONTRACT_LAST, preferred_element_type=F32
        )
        sums = jnp.where(diagonal, sums, 0.0)
        folded = sums[:, :LANES]
        for low_lane in range(LANES, depth, LANES):
            folded = folded + sums[:, low_lane : low_lane + LANES]
        folded = folded + pltpu.roll(folded, HEAD_LANES, 1)
        part[low : low + per_group, :] = jnp.where(
            lane < HEAD_LANES, folded, jnp.where(lane < 96, top, total)
        )
    key_new = dot(rounded, key_weight[...]).astype(BF16)
    value_new = dot(rounded, value_weight[...]).astype(BF16)
    product = query.astype(F32) * key_new.astype(F32)
    mine = iota((rows, LANES), 1) // HEAD_LANES == iota((rows, LANES), 0) % local_heads
    own = jnp.sum(jnp.where(mine, exact_dot(spread, product), 0.0), axis=1, keepdims=True) * scale
    value_rows = jnp.where(mine, dot(spread_short, value_new), 0.0)
    value_rows = value_rows + pltpu.roll(value_rows, HEAD_LANES, 1)
    newest[...] = jnp.where(iota((rows, LANES), 1) < HEAD_LANES, value_rows, own)


def merge_kernel(local_heads, count, *refs):
    parts = [ref[...] for ref in refs[:count]]
    newest, out_weight, short, full = refs[count:]
    rows = newest.shape[0]
    lane = iota((rows, LANES), 1)

    def pick(array, index):
        return jnp.sum(jnp.where(lane == index, array, 0.0), axis=1, keepdims=True)

    tops = [pick(array, HEAD_LANES) for array in parts]
    totals = [pick(array, 96) for array in parts]
    latest = newest[...]
    own = pick(latest, HEAD_LANES)
    peak = own
    for top in tops:
        peak = jnp.maximum(peak, top)
    own_factor = jnp.exp(own - peak)
    numer = latest * own_factor
    denom = own_factor
    for array, top, total in zip(parts, tops, totals):
        factor = jnp.exp(top - peak)
        numer = numer + array * factor
        denom = denom + total * factor
    ratio = jnp.where(lane < HEAD_LANES, numer / denom, 0.0)
    ratio = ratio + pltpu.roll(ratio, HEAD_LANES, 1)
    mine = lane // HEAD_LANES == iota((rows, LANES), 0) % local_heads
    ratio = jnp.where(mine, ratio, 0.0).astype(BF16)
    batch = rows // local_heads
    gather = (iota((batch, rows), 1) // local_heads == iota((batch, rows), 0)).astype(BF16)
    attention = dot(gather, ratio).astype(BF16)
    product = dot(attention, out_weight[...])
    full[...] = product
    short[...] = product.astype(BF16)


def add_kernel(*refs):
    total = refs[0][...]
    for ref in refs[1:-1]:
        total = total + ref[...].astype(F32)
    refs[-1][...] = total


def up_kernel(kv, tp, one, two, blocks, gain, up_weight, short, full, piece, middle, mixed):
    first = lax.axis_index("kv") * tp
    total = one[...] + two[...]
    batch = total.shape[0]
    squares = jnp.zeros((batch, LANES), F32)
    for block in range(tp):
        low = block * LANES
        value = (blocks[first + block].astype(F32) + total[:, low : low + LANES]).astype(BF16)
        wide = value.astype(F32)
        middle[block] = wide
        squares = squares + wide * wide
        mixed[:, low : low + LANES] = (wide * gain[pl.ds(first + block, 1), :]).astype(BF16)
    piece[...] = middle[lax.axis_index("tp")]
    product = dot(mixed[...], up_weight[...])
    width = product.shape[1]
    full[...] = product
    short[:, :width] = product.astype(BF16)
    rest = jnp.sum(squares, axis=1, keepdims=True)
    lane = iota((batch, LANES), 1)
    tail = jnp.zeros((batch, LANES), F32)
    for index in range(3):
        digit = rest.astype(BF16).astype(F32)
        tail = jnp.where(lane == index, digit, tail)
        rest = rest - digit
    short[:, width:] = tail.astype(BF16)


def down_kernel(tp, size, count, *refs):
    full, short = refs[0], refs[1]
    others = refs[2 : 1 + count]
    down_weight, keep, send, shares = refs[1 + count :]
    width = full.shape[1]
    total = full[...]
    tail = short[:, width:].astype(F32)
    for ref in others:
        total = total + ref[:, :width].astype(F32)
        tail = tail + ref[:, width:].astype(F32)
    mean = jnp.sum(tail, axis=1, keepdims=True) / size
    active = jnp.maximum(total * lax.rsqrt(mean + EPS), 0.0)
    product = dot((active * active).astype(BF16), down_weight[...])
    for block in range(tp):
        shares[block] = product[:, block * LANES : (block + 1) * LANES]
    core = lax.rem(lax.axis_index("tp"), 2)
    for pair in range(tp // 2):
        keep[pair] = shares[2 * pair + core]
        send[pair] = shares[2 * pair + 1 - core]


def split_kernel(pairs, keep, other, *refs):
    outs, own, shares = refs[:-2], refs[-2], refs[-1]
    shares[...] = keep[...] + other[...]
    place = lax.div(lax.axis_index("tp"), 2)
    own[...] = shares[place]
    for step in range(1, pairs):
        outs[step - 1][...] = shares[lax.rem(place + step, pairs)].astype(BF16)


def last_kernel(*refs):
    total = refs[0][...]
    for ref in refs[1:-1]:
        total = total + ref[...].astype(F32)
    refs[-1][...] = total.astype(BF16)


def shards(
    kv,
    tp,
    stream,
    mixer_gain,
    query_weight,
    key_weight,
    value_weight,
    forget_weight,
    forget_bias,
    key_cache,
    value_cache,
    past_decay,
    out_weight,
    channel_gain,
    up_weight,
    down_weight,
):
    batch, piece_width = stream.shape
    _, local_heads, places, head_size = key_cache.shape
    rows = batch * local_heads
    fits = (
        piece_width == LANES
        and head_size == HEAD_LANES
        and local_heads == LANES // HEAD_LANES
        and tp % 2 == 0
        and rows % 8 == 0
        and places % LANES == 0
        and out_weight.shape[1] == tp * LANES
    )
    if not fits:
        return shards_general(
            stream,
            mixer_gain,
            query_weight,
            key_weight,
            value_weight,
            forget_weight,
            forget_bias,
            key_cache,
            value_cache,
            past_decay,
            out_weight,
            channel_gain,
            up_weight,
            down_weight,
        )
    count = kv * tp
    size = count * piece_width
    groups = rows // 8
    depth = 8 * head_size
    (fanned,) = kernel_call(
        fan_kernel,
        [shape_of((count, batch, piece_width), BF16)],
        (stream,),
        cost=pl.CostEstimate(flops=40_000_000_000, bytes_accessed=0, transcendentals=0),
    )
    blocks = lax.all_to_all(fanned, ("kv", "tp"), 0, 0)
    keys = jnp.swapaxes(key_cache, 2, 3).reshape(groups, depth, places)
    values = jnp.swapaxes(value_cache, 2, 3).reshape(groups, depth, places)
    heads = forget_bias.shape[0]
    part, newest = kernel_call(
        functools.partial(attention_kernel, local_heads),
        [shape_of((rows, LANES), F32)] * 2,
        (
            blocks,
            mixer_gain.reshape(count, LANES),
            query_weight,
            key_weight,
            value_weight,
            forget_weight.T,
            forget_bias.reshape(1, heads),
            keys,
            values,
            past_decay,
        ),
        scratch=[pltpu.VMEM((batch, size), BF16)],
    )
    def turn(array, axis, length, step, stride=1):
        total = length * stride
        return lax.ppermute(array, axis, [(i, (i + step * stride) % total) for i in range(total)])

    def swap(array):
        return lax.ppermute(array, "tp", [(i, i ^ 1) for i in range(tp)])

    pairs = tp // 2
    others = [turn(part, "kv", kv, step) for step in range(1, kv)]
    block_width = out_weight.shape[1]
    short, full = kernel_call(
        functools.partial(merge_kernel, local_heads, kv),
        [shape_of((batch, block_width), BF16), shape_of((batch, block_width), F32)],
        (part, *others, newest, out_weight),
    )
    others = [turn(short, "tp", pairs, step, 2) for step in range(1, pairs)]
    (column_sum,) = kernel_call(add_kernel, [shape_of((batch, block_width), F32)], (full, *others))
    width = up_weight.shape[1]
    short, full, piece = kernel_call(
        functools.partial(up_kernel, kv, tp),
        [
            shape_of((batch, width + LANES), BF16),
            shape_of((batch, width), F32),
            shape_of((batch, LANES), F32),
        ],
        (column_sum, swap(column_sum), blocks, channel_gain.reshape(count, LANES), up_weight),
        scratch=[pltpu.VMEM((tp, batch, LANES), F32), pltpu.VMEM((batch, block_width), BF16)],
    )
    others = [turn(short, "kv", kv, step) for step in range(1, kv)]
    keep, send = kernel_call(
        functools.partial(down_kernel, tp, size, kv),
        [shape_of((pairs, batch, LANES), F32)] * 2,
        (full, short, *others, down_weight),
        scratch=[pltpu.VMEM((tp, batch, LANES), F32)],
    )
    *shares, own = kernel_call(
        functools.partial(split_kernel, pairs),
        [shape_of((batch, LANES), BF16)] * (pairs - 1) + [shape_of((batch, LANES), F32)],
        (keep, swap(send)),
        scratch=[pltpu.VMEM((pairs, batch, LANES), F32)],
    )
    others = [turn(shares[step - 1], "tp", pairs, step, 2) for step in range(1, pairs)]
    (updated,) = kernel_call(
        last_kernel, [shape_of((batch, LANES), BF16)], (piece, own, *others)
    )
    return updated


def solution(mesh):
    return jax.shard_map(
        functools.partial(shards, mesh.shape["kv"], mesh.shape["tp"]),
        mesh=mesh,
        in_specs=(
            P(None, ("kv", "tp")),
            P(),
            P(None, "tp"),
            P(None, "tp"),
            P(None, "tp"),
            P(),
            P(),
            P(None, "tp", "kv", None),
            P(None, "tp", "kv", None),
            P(None, "tp", "kv"),
            P("tp", "kv"),
            P(),
            P("kv", "tp"),
            P("tp", "kv"),
        ),
        out_specs=P(None, ("kv", "tp")),
        check_vma=False,
    )
```

```python
import functools

import jax
import jax.numpy as jnp
from jax import lax
from jax.experimental import pallas as pl
from jax.experimental.pallas import tpu as pltpu
from jax.sharding import PartitionSpec as P

D = 4096


EPS = 1e-06


def combined_all(part, axis, combine):
    gathered = jax.tree.map(lambda a: lax.all_gather(a, axis), part)

    def take(source):
        return jax.tree.map(lambda a: lax.dynamic_index_in_dim(a, source, 0, False), gathered)

    return lax.fori_loop(
        1, lax.axis_size(axis), lambda source, state: combine(state, take(source)), take(0)
    )


def rms_scale(values, gain):
    widened = values.astype(jnp.float32)
    inverse = lax.rsqrt(jnp.mean(widened * widened, axis=-1, keepdims=True) + EPS)
    return (widened * inverse * gain).astype(jnp.bfloat16)


def merge_parts(earlier, later):
    top_one, total_one, sums_one = earlier
    top_two, total_two, sums_two = later
    highest = jnp.maximum(top_one, top_two)
    factor_one = jnp.exp(top_one - highest)
    factor_two = jnp.exp(top_two - highest)
    return (
        highest,
        total_one * factor_one + total_two * factor_two,
        sums_one * factor_one[..., None] + sums_two * factor_two[..., None],
    )


def squared_relu(values):
    return jnp.square(jax.nn.relu(values)).astype(jnp.bfloat16)


def row_squares(values):
    widened = values.astype(jnp.float32)
    return jnp.sum(widened * widened, axis=1)


def shards_general(
    stream,
    mixer_gain,
    query_weight,
    key_weight,
    value_weight,
    forget_weight,
    forget_bias,
    key_cache,
    value_cache,
    past_decay,
    out_weight,
    channel_gain,
    up_weight,
    down_weight,
):
    batch_rows = stream.shape[0]
    local_heads = key_cache.shape[1]
    head_size = key_cache.shape[3]
    scale_factor = float(head_size) ** (-0.5)
    gathered = lax.all_gather(stream, ("kv", "tp"), axis=1, tiled=True)
    normed = rms_scale(gathered, mixer_gain)
    queries = jnp.dot(normed, query_weight, preferred_element_type=jnp.float32).astype(jnp.bfloat16)
    keys_new = jnp.dot(normed, key_weight, preferred_element_type=jnp.float32).astype(jnp.bfloat16)
    values_new = jnp.dot(normed, value_weight, preferred_element_type=jnp.float32).astype(
        jnp.bfloat16
    )
    forget_all = jax.nn.log_sigmoid(
        jnp.dot(normed, forget_weight, preferred_element_type=jnp.float32) + forget_bias
    )
    forget = lax.dynamic_slice_in_dim(
        forget_all, lax.axis_index("tp") * local_heads, local_heads, 1
    )
    query_heads = queries.reshape(batch_rows, local_heads, head_size)
    scores = (
        jnp.einsum("bhd,bhpd->bhp", query_heads, key_cache, preferred_element_type=jnp.float32)
        * scale_factor
        + forget[..., None]
        + past_decay
    )
    highest = jnp.max(scores, axis=-1)
    weights = jnp.exp(scores - highest[..., None]).astype(jnp.bfloat16)
    totals = jnp.sum(weights.astype(jnp.float32), axis=-1)
    sums = jnp.einsum("bhp,bhpd->bhd", weights, value_cache, preferred_element_type=jnp.float32)
    highest, totals, sums = combined_all((highest, totals, sums), "kv", merge_parts)
    key_heads = keys_new.reshape(batch_rows, local_heads, head_size).astype(jnp.float32)
    value_heads = values_new.reshape(batch_rows, local_heads, head_size).astype(jnp.float32)
    own = jnp.sum(query_heads.astype(jnp.float32) * key_heads, axis=-1) * scale_factor
    peak = jnp.maximum(highest, own)
    cache_factor = jnp.exp(highest - peak)
    own_factor = jnp.exp(own - peak)
    numer = sums * cache_factor[..., None] + value_heads * own_factor[..., None]
    denom = totals * cache_factor + own_factor
    attention = (
        (numer / denom[..., None]).astype(jnp.bfloat16).reshape(batch_rows, local_heads * head_size)
    )
    partial_value = jnp.dot(attention, out_weight, preferred_element_type=jnp.float32)
    piece_width = stream.shape[1]
    block_width = partial_value.shape[1]
    block_sum = lax.psum(partial_value, "tp")
    own_block = lax.dynamic_slice_in_dim(
        gathered, lax.axis_index("kv") * block_width, block_width, 1
    )
    middle_block = (own_block.astype(jnp.float32) + block_sum).astype(jnp.bfloat16)
    squares = lax.psum(row_squares(middle_block), "kv")
    middle_piece = lax.dynamic_slice_in_dim(
        middle_block, lax.axis_index("tp") * piece_width, piece_width, 1
    )
    inverse = lax.rsqrt(squares / D + EPS)
    gain_block = lax.dynamic_slice_in_dim(
        channel_gain, lax.axis_index("kv") * block_width, block_width, 0
    )
    mixed_block = (
        middle_block.astype(jnp.float32) * inverse[:, None] * gain_block[None, :]
    ).astype(jnp.bfloat16)
    up_partial = jnp.dot(mixed_block, up_weight, preferred_element_type=jnp.float32)
    hidden = squared_relu(lax.psum(up_partial, "kv"))
    down_partial = jnp.dot(hidden, down_weight, preferred_element_type=jnp.float32)
    reduced = lax.psum_scatter(down_partial, "tp", scatter_dimension=1, tiled=True)
    return (middle_piece.astype(jnp.float32) + reduced).astype(jnp.bfloat16)


LANES = 128
HEAD_LANES = 64
PACK = 16
F32 = jnp.float32
BF16 = jnp.bfloat16
CONTRACT_LAST = (((1,), (1,)), ((), ()))


def iota(shape, axis):
    return lax.broadcasted_iota(jnp.int32, shape, axis)


def dot(one, two):
    return jnp.dot(one, two, preferred_element_type=F32)


def kernel_call(body, out_shapes, arguments, scratch=(), limit=8, cost=None):
    return pl.pallas_call(
        body,
        out_shape=tuple(out_shapes),
        in_specs=[pl.BlockSpec(memory_space=pltpu.VMEM)] * len(arguments),
        out_specs=tuple(pl.BlockSpec(memory_space=pltpu.VMEM) for _ in out_shapes),
        scratch_shapes=list(scratch),
        cost_estimate=cost,
        compiler_params=pltpu.CompilerParams(vmem_limit_bytes=limit << 20),
    )(*arguments)


def shape_of(shape, dtype):
    return jax.ShapeDtypeStruct(shape, dtype)


def fan_kernel(piece, copies):
    value = piece[...]
    for index in range(copies.shape[0]):
        copies[index] = value


def attention_kernel(
    local_heads,
    blocks,
    gain,
    query_weight,
    forget_weight,
    forget_bias,
    keys,
    values,
    decay,
    part,
    normed,
    queries,
):
    groups, depth, _ = keys.shape
    count, batch, _ = blocks.shape
    squares = jnp.zeros((batch, LANES), F32)
    for block in range(count):
        wide = blocks[block].astype(F32)
        squares = squares + wide * wide
    mean = jnp.sum(squares, axis=1, keepdims=True) / (count * LANES)
    inverse = lax.rsqrt(mean + EPS)
    for block in range(count):
        scaled = blocks[block].astype(F32) * inverse * gain[block : block + 1, :]
        normed[:, block * LANES : (block + 1) * LANES] = scaled.astype(BF16)
    rounded = normed[...]
    query = dot(rounded, query_weight[...]).astype(BF16)
    queries[...] = query
    query = query.astype(F32)
    logits = lax.dot_general(
        rounded, forget_weight[...], CONTRACT_LAST, preferred_element_type=F32
    )
    logits = logits + forget_bias[...]
    forget = jnp.minimum(logits, 0.0) - jnp.log1p(jnp.exp(-jnp.abs(logits)))
    first_head = lax.axis_index("tp") * local_heads
    head = iota(forget.shape, 1)
    forgets = [
        jnp.sum(jnp.where(head == first_head + index, forget, 0.0), axis=1, keepdims=True)
        for index in range(local_heads)
    ]
    per_group = batch * local_heads // groups
    batches = batch // groups
    place_of = [(row // local_heads, row % local_heads) for row in range(per_group)]
    tile_lane = iota((per_group, LANES), 1)
    tile_row = iota((per_group, LANES), 0)
    column = iota((HEAD_LANES, LANES), 1)
    columns = jnp.zeros((HEAD_LANES, LANES), F32)
    stats = jnp.zeros((per_group, LANES), F32)
    scale = float(HEAD_LANES) ** (-0.5)
    for group in range(groups):
        base = group * batches
        rows = jnp.concatenate([query[base + b : base + b + 1] for b, _ in place_of], axis=0)
        wide = [
            jnp.where((tile_lane + low) // HEAD_LANES == tile_row, rows, 0.0)
            for low in range(0, depth, LANES)
        ]
        fade = jnp.concatenate([forgets[h][base + b : base + b + 1] for b, h in place_of], axis=0)
        wide = jnp.concatenate(wide, axis=1).astype(BF16)
        scores = dot(wide, keys[group]) * scale + fade
        scores = scores + decay[base : base + batches].reshape(per_group, -1)
        top = jnp.max(scores, axis=1, keepdims=True)
        short = jnp.exp(scores - top).astype(BF16).astype(F32)
        total = jnp.sum(short, axis=1, keepdims=True)
        for row, (b, h) in enumerate(place_of):
            mixed = jnp.zeros((HEAD_LANES, LANES), F32)
            for place in range(0, short.shape[1], LANES):
                value = values[
                    group, row * HEAD_LANES : (row + 1) * HEAD_LANES, place : place + LANES
                ]
                mixed = mixed + value.astype(F32) * short[row : row + 1, place : place + LANES]
            summed = jnp.sum(mixed, axis=1, keepdims=True)
            columns = jnp.where(column == h * batch + base + b, summed, columns)
        stats = jnp.where(tile_lane == group, top, stats)
        stats = jnp.where(tile_lane == HEAD_LANES + group, total, stats)
    flat = jnp.concatenate([columns, columns], axis=0).T
    lane = iota((batch, LANES), 1)
    part[:batch, :] = jnp.where(lane < HEAD_LANES, flat[:batch], flat[batch : 2 * batch])
    part[batch:, :] = stats


def newest_kernel(normed, queries, key_weight, value_weight, newest, own):
    rounded = normed[...]
    key_new = dot(rounded, key_weight[...]).astype(BF16)
    newest[...] = dot(rounded, value_weight[...]).astype(BF16).astype(F32)
    product = queries[...].astype(F32) * key_new.astype(F32)
    low = iota(product.shape, 1) < HEAD_LANES
    scale = float(HEAD_LANES) ** (-0.5)
    one = jnp.sum(jnp.where(low, product, 0.0), axis=1, keepdims=True)
    two = jnp.sum(jnp.where(low, 0.0, product), axis=1, keepdims=True)
    own[...] = jnp.where(low, one, two) * scale


def merge_kernel(local_heads, groups, count, *refs):
    newest, owns, out_weight, short, full = refs[count:]
    batch = newest.shape[0]
    batches = batch // groups
    lane = iota((batch, LANES), 1)
    row = iota((batch, LANES), 0)
    low = lane < HEAD_LANES

    def spread(stats, offset):
        found = []
        for head in range(local_heads):
            picked = stats[head : head + 1]
            for b in range(1, batches):
                index = b * local_heads + head
                picked = jnp.where(row % batches == b, stats[index : index + 1], picked)
            picked = jnp.where(lane == offset + row // batches, picked, 0.0)
            found.append(jnp.sum(picked, axis=1, keepdims=True))
        return jnp.where(low, found[0], found[1])

    tops = [spread(ref[batch:, :], 0) for ref in refs[:count]]
    totals = [spread(ref[batch:, :], HEAD_LANES) for ref in refs[:count]]
    own = owns[...]
    peak = own
    for top in tops:
        peak = jnp.maximum(peak, top)
    own_factor = jnp.exp(own - peak)
    numer = newest[...] * own_factor
    denom = own_factor
    for ref, top, total in zip(refs, tops, totals):
        factor = jnp.exp(top - peak)
        numer = numer + ref[:batch, :] * factor
        denom = denom + total * factor
    product = dot((numer / denom).astype(BF16), out_weight[...])
    full[...] = product
    short[...] = product.astype(BF16)


def add_kernel(*refs):
    total = refs[0][...]
    for ref in refs[1:-1]:
        total = total + ref[...].astype(F32)
    refs[-1][...] = total


def up_kernel(kv, tp, one, two, blocks, gain, up_weight, short, full, piece, middle, mixed):
    first = lax.axis_index("kv") * tp
    total = one[...] + two[...]
    batch = total.shape[0]
    squares = jnp.zeros((batch, LANES), F32)
    for block in range(tp):
        low = block * LANES
        value = (blocks[first + block].astype(F32) + total[:, low : low + LANES]).astype(BF16)
        wide = value.astype(F32)
        middle[block] = wide
        squares = squares + wide * wide
        mixed[:, low : low + LANES] = (wide * gain[pl.ds(first + block, 1), :]).astype(BF16)
    piece[...] = middle[lax.axis_index("tp")]
    product = dot(mixed[...], up_weight[...])
    width = product.shape[1]
    full[...] = product
    for block in range(width // LANES):
        short[block * batch : (block + 1) * batch, :] = product[
            :, block * LANES : (block + 1) * LANES
        ].astype(BF16)
    rest = jnp.sum(squares, axis=1, keepdims=True)
    lane = iota((batch, LANES), 1)
    rest = jnp.where(lane == iota((batch, LANES), 0), rest, 0.0)
    rest = jnp.sum(rest, axis=0, keepdims=True)
    row = iota((PACK, LANES), 0)
    tail = jnp.zeros((PACK, LANES), F32)
    for index in range(3):
        digit = rest.astype(BF16).astype(F32)
        tail = jnp.where(row == index, digit, tail)
        rest = rest - digit
    short[short.shape[0] - PACK :, :] = tail.astype(BF16)


def down_kernel(tp, size, count, *refs):
    full, short = refs[0], refs[1]
    others = refs[2 : 1 + count]
    down_weight, keep, send, shares = refs[1 + count :]
    batch, width = full.shape
    height = width // LANES * batch
    tail = short[height:, :].astype(F32)
    for ref in others:
        tail = tail + ref[height:, :].astype(F32)
    tail = jnp.sum(tail, axis=0, keepdims=True)
    lane = iota((batch, LANES), 1)
    tail = jnp.where(lane == iota((batch, LANES), 0), tail, 0.0)
    inverse = lax.rsqrt(jnp.sum(tail, axis=1, keepdims=True) / size + EPS)
    pieces = []
    for block in range(width // LANES):
        total = full[:, block * LANES : (block + 1) * LANES]
        for ref in others:
            total = total + ref[block * batch : (block + 1) * batch, :].astype(F32)
        active = jnp.maximum(total * inverse, 0.0)
        pieces.append((active * active).astype(BF16))
    product = dot(jnp.concatenate(pieces, axis=1), down_weight[...])
    for block in range(tp):
        shares[block] = product[:, block * LANES : (block + 1) * LANES]
    core = lax.rem(lax.axis_index("tp"), 2)
    for pair in range(tp // 2):
        keep[pair] = shares[2 * pair + core]
        send[pair] = shares[2 * pair + 1 - core]


def split_kernel(pairs, keep, other, *refs):
    outs, own, shares = refs[:-2], refs[-2], refs[-1]
    shares[...] = keep[...] + other[...]
    place = lax.div(lax.axis_index("tp"), 2)
    own[...] = shares[place]
    for step in range(1, pairs):
        outs[step - 1][...] = shares[lax.rem(place + step, pairs)].astype(BF16)


def last_kernel(*refs):
    total = refs[0][...]
    for ref in refs[1:-1]:
        total = total + ref[...].astype(F32)
    refs[-1][...] = total.astype(BF16)


def shards(
    kv,
    tp,
    stream,
    mixer_gain,
    query_weight,
    key_weight,
    value_weight,
    forget_weight,
    forget_bias,
    key_cache,
    value_cache,
    past_decay,
    out_weight,
    channel_gain,
    up_weight,
    down_weight,
):
    batch, piece_width = stream.shape
    _, local_heads, places, head_size = key_cache.shape
    rows = batch * local_heads
    fits = (
        piece_width == LANES
        and head_size == HEAD_LANES
        and local_heads == LANES // HEAD_LANES
        and tp % 2 == 0
        and kv & (kv - 1) == 0
        and rows == HEAD_LANES
        and batch % PACK == 0
        and up_weight.shape[1] % LANES == 0
        and places % LANES == 0
        and out_weight.shape[1] == tp * LANES
    )
    if not fits:
        return shards_general(
            stream,
            mixer_gain,
            query_weight,
            key_weight,
            value_weight,
            forget_weight,
            forget_bias,
            key_cache,
            value_cache,
            past_decay,
            out_weight,
            channel_gain,
            up_weight,
            down_weight,
        )
    count = kv * tp
    size = count * piece_width
    groups = rows // 8
    depth = 8 * head_size
    (fanned,) = kernel_call(
        fan_kernel,
        [shape_of((count, batch, piece_width), BF16)],
        (stream,),
        cost=pl.CostEstimate(flops=40_000_000_000, bytes_accessed=0, transcendentals=0),
    )
    blocks = lax.all_to_all(fanned, ("kv", "tp"), 0, 0)
    keys = jnp.swapaxes(key_cache, 2, 3).reshape(groups, depth, places)
    values = jnp.swapaxes(value_cache, 2, 3).reshape(groups, depth, places)
    heads = forget_bias.shape[0]
    part, normed, queries = kernel_call(
        functools.partial(attention_kernel, local_heads),
        [
            shape_of((batch + 8, LANES), F32),
            shape_of((batch, size), BF16),
            shape_of((batch, LANES), BF16),
        ],
        (
            blocks,
            mixer_gain.reshape(count, LANES),
            query_weight,
            forget_weight.T,
            forget_bias.reshape(1, heads),
            keys,
            values,
            past_decay,
        ),
    )
    newest, owns = kernel_call(
        newest_kernel,
        [shape_of((batch, LANES), F32)] * 2,
        (normed, queries, key_weight, value_weight),
    )
    def trade(array, step):
        return lax.ppermute(array, "kv", [(i, i ^ step) for i in range(kv)])

    def turn(array, step):
        return lax.ppermute(array, "tp", [(i, (i + 2 * step) % tp) for i in range(tp)])

    def swap(array):
        return lax.ppermute(array, "tp", [(i, i ^ 1) for i in range(tp)])

    pairs = tp // 2
    others = [trade(part, step) for step in range(1, kv)]
    block_width = out_weight.shape[1]
    short, full = kernel_call(
        functools.partial(merge_kernel, local_heads, groups, kv),
        [shape_of((batch, block_width), BF16), shape_of((batch, block_width), F32)],
        (part, *others, newest, owns, out_weight),
    )
    others = [turn(short, step) for step in range(1, pairs)]
    (column_sum,) = kernel_call(add_kernel, [shape_of((batch, block_width), F32)], (full, *others))
    width = up_weight.shape[1]
    short, full, piece = kernel_call(
        functools.partial(up_kernel, kv, tp),
        [
            shape_of((batch * width // LANES + PACK, LANES), BF16),
            shape_of((batch, width), F32),
            shape_of((batch, LANES), F32),
        ],
        (column_sum, swap(column_sum), blocks, channel_gain.reshape(count, LANES), up_weight),
        scratch=[pltpu.VMEM((tp, batch, LANES), F32), pltpu.VMEM((batch, block_width), BF16)],
    )
    others = [trade(short, step) for step in range(1, kv)]
    keep, send = kernel_call(
        functools.partial(down_kernel, tp, size, kv),
        [shape_of((pairs, batch, LANES), F32)] * 2,
        (full, short, *others, down_weight),
        scratch=[pltpu.VMEM((tp, batch, LANES), F32)],
    )
    *shares, own = kernel_call(
        functools.partial(split_kernel, pairs),
        [shape_of((batch, LANES), BF16)] * (pairs - 1) + [shape_of((batch, LANES), F32)],
        (keep, swap(send)),
        scratch=[pltpu.VMEM((pairs, batch, LANES), F32)],
    )
    others = [turn(shares[step - 1], step) for step in range(1, pairs)]
    (updated,) = kernel_call(
        last_kernel, [shape_of((batch, LANES), BF16)], (piece, own, *others)
    )
    return updated


def solution(mesh):
    return jax.shard_map(
        functools.partial(shards, mesh.shape["kv"], mesh.shape["tp"]),
        mesh=mesh,
        in_specs=(
            P(None, ("kv", "tp")),
            P(),
            P(None, "tp"),
            P(None, "tp"),
            P(None, "tp"),
            P(),
            P(),
            P(None, "tp", "kv", None),
            P(None, "tp", "kv", None),
            P(None, "tp", "kv"),
            P("tp", "kv"),
            P(),
            P("kv", "tp"),
            P("tp", "kv"),
        ),
        out_specs=P(None, ("kv", "tp")),
        check_vma=False,
    )
```

```python
import functools

import jax
import jax.numpy as jnp
from jax import lax
from jax.experimental import pallas as pl
from jax.experimental.pallas import tpu as pltpu
from jax.sharding import PartitionSpec as P

D = 4096


EPS = 1e-06


def combined_all(part, axis, combine):
    gathered = jax.tree.map(lambda a: lax.all_gather(a, axis), part)

    def take(source):
        return jax.tree.map(lambda a: lax.dynamic_index_in_dim(a, source, 0, False), gathered)

    return lax.fori_loop(
        1, lax.axis_size(axis), lambda source, state: combine(state, take(source)), take(0)
    )


def rms_scale(values, gain):
    widened = values.astype(jnp.float32)
    inverse = lax.rsqrt(jnp.mean(widened * widened, axis=-1, keepdims=True) + EPS)
    return (widened * inverse * gain).astype(jnp.bfloat16)


def merge_parts(earlier, later):
    top_one, total_one, sums_one = earlier
    top_two, total_two, sums_two = later
    highest = jnp.maximum(top_one, top_two)
    factor_one = jnp.exp(top_one - highest)
    factor_two = jnp.exp(top_two - highest)
    return (
        highest,
        total_one * factor_one + total_two * factor_two,
        sums_one * factor_one[..., None] + sums_two * factor_two[..., None],
    )


def squared_relu(values):
    return jnp.square(jax.nn.relu(values)).astype(jnp.bfloat16)


def row_squares(values):
    widened = values.astype(jnp.float32)
    return jnp.sum(widened * widened, axis=1)


def shards_general(
    stream,
    mixer_gain,
    query_weight,
    key_weight,
    value_weight,
    forget_weight,
    forget_bias,
    key_cache,
    value_cache,
    past_decay,
    out_weight,
    channel_gain,
    up_weight,
    down_weight,
):
    batch_rows = stream.shape[0]
    local_heads = key_cache.shape[1]
    head_size = key_cache.shape[3]
    scale_factor = float(head_size) ** (-0.5)
    gathered = lax.all_gather(stream, ("kv", "tp"), axis=1, tiled=True)
    normed = rms_scale(gathered, mixer_gain)
    queries = jnp.dot(normed, query_weight, preferred_element_type=jnp.float32).astype(jnp.bfloat16)
    keys_new = jnp.dot(normed, key_weight, preferred_element_type=jnp.float32).astype(jnp.bfloat16)
    values_new = jnp.dot(normed, value_weight, preferred_element_type=jnp.float32).astype(
        jnp.bfloat16
    )
    forget_all = jax.nn.log_sigmoid(
        jnp.dot(normed, forget_weight, preferred_element_type=jnp.float32) + forget_bias
    )
    forget = lax.dynamic_slice_in_dim(
        forget_all, lax.axis_index("tp") * local_heads, local_heads, 1
    )
    query_heads = queries.reshape(batch_rows, local_heads, head_size)
    scores = (
        jnp.einsum("bhd,bhpd->bhp", query_heads, key_cache, preferred_element_type=jnp.float32)
        * scale_factor
        + forget[..., None]
        + past_decay
    )
    highest = jnp.max(scores, axis=-1)
    weights = jnp.exp(scores - highest[..., None]).astype(jnp.bfloat16)
    totals = jnp.sum(weights.astype(jnp.float32), axis=-1)
    sums = jnp.einsum("bhp,bhpd->bhd", weights, value_cache, preferred_element_type=jnp.float32)
    highest, totals, sums = combined_all((highest, totals, sums), "kv", merge_parts)
    key_heads = keys_new.reshape(batch_rows, local_heads, head_size).astype(jnp.float32)
    value_heads = values_new.reshape(batch_rows, local_heads, head_size).astype(jnp.float32)
    own = jnp.sum(query_heads.astype(jnp.float32) * key_heads, axis=-1) * scale_factor
    peak = jnp.maximum(highest, own)
    cache_factor = jnp.exp(highest - peak)
    own_factor = jnp.exp(own - peak)
    numer = sums * cache_factor[..., None] + value_heads * own_factor[..., None]
    denom = totals * cache_factor + own_factor
    attention = (
        (numer / denom[..., None]).astype(jnp.bfloat16).reshape(batch_rows, local_heads * head_size)
    )
    partial_value = jnp.dot(attention, out_weight, preferred_element_type=jnp.float32)
    piece_width = stream.shape[1]
    block_width = partial_value.shape[1]
    block_sum = lax.psum(partial_value, "tp")
    own_block = lax.dynamic_slice_in_dim(
        gathered, lax.axis_index("kv") * block_width, block_width, 1
    )
    middle_block = (own_block.astype(jnp.float32) + block_sum).astype(jnp.bfloat16)
    squares = lax.psum(row_squares(middle_block), "kv")
    middle_piece = lax.dynamic_slice_in_dim(
        middle_block, lax.axis_index("tp") * piece_width, piece_width, 1
    )
    inverse = lax.rsqrt(squares / D + EPS)
    gain_block = lax.dynamic_slice_in_dim(
        channel_gain, lax.axis_index("kv") * block_width, block_width, 0
    )
    mixed_block = (
        middle_block.astype(jnp.float32) * inverse[:, None] * gain_block[None, :]
    ).astype(jnp.bfloat16)
    up_partial = jnp.dot(mixed_block, up_weight, preferred_element_type=jnp.float32)
    hidden = squared_relu(lax.psum(up_partial, "kv"))
    down_partial = jnp.dot(hidden, down_weight, preferred_element_type=jnp.float32)
    reduced = lax.psum_scatter(down_partial, "tp", scatter_dimension=1, tiled=True)
    return (middle_piece.astype(jnp.float32) + reduced).astype(jnp.bfloat16)


LANES = 128
HEAD_LANES = 64
PACK = 16
WIDE = 256
AHEAD = 1
F32 = jnp.float32
BF16 = jnp.bfloat16
CONTRACT_LAST = (((1,), (1,)), ((), ()))


def iota(shape, axis):
    return lax.broadcasted_iota(jnp.int32, shape, axis)


def dot(one, two):
    return jnp.dot(one, two, preferred_element_type=F32)


def kernel_call(body, out_shapes, arguments, scratch=(), limit=8, cost=None, aliases=None):
    return pl.pallas_call(
        body,
        out_shape=tuple(out_shapes),
        in_specs=[pl.BlockSpec(memory_space=pltpu.VMEM)] * len(arguments),
        out_specs=tuple(pl.BlockSpec(memory_space=pltpu.VMEM) for _ in out_shapes),
        scratch_shapes=list(scratch),
        cost_estimate=cost,
        input_output_aliases=aliases or {},
        compiler_params=pltpu.CompilerParams(vmem_limit_bytes=limit << 20),
    )(*arguments)


def shape_of(shape, dtype):
    return jax.ShapeDtypeStruct(shape, dtype)


def fan_kernel(piece, copies):
    value = piece[...]
    for index in range(copies.shape[0]):
        copies[index] = value


def hold_kernel(copies, same):
    same[0] = copies[0]


def attention_kernel(
    local_heads,
    blocks,
    gain,
    query_weight,
    forget_weight,
    forget_bias,
    keys,
    values,
    decay,
    part,
    normed,
    queries,
    spread,
):
    groups, depth, _ = keys.shape
    count, batch, _ = blocks.shape
    squares = jnp.zeros((batch, LANES), F32)
    for block in range(count):
        wide = blocks[block].astype(F32)
        squares = squares + wide * wide
    mean = jnp.sum(squares, axis=1, keepdims=True) / (count * LANES)
    inverse = lax.rsqrt(mean + EPS)
    for block in range(count):
        scaled = blocks[block].astype(F32) * inverse * gain[block : block + 1, :]
        normed[:, block * LANES : (block + 1) * LANES] = scaled.astype(BF16)
    rounded = normed[...]
    query = dot(rounded, query_weight[...]).astype(BF16)
    queries[...] = query
    query = query.astype(F32)
    logits = lax.dot_general(
        rounded, forget_weight[...], CONTRACT_LAST, preferred_element_type=F32
    )
    logits = logits + forget_bias[...]
    forget = jnp.minimum(logits, 0.0) - jnp.log1p(jnp.exp(-jnp.abs(logits)))
    first_head = lax.axis_index("tp") * local_heads
    head = iota(forget.shape, 1)
    forgets = [
        jnp.sum(jnp.where(head == first_head + index, forget, 0.0), axis=1, keepdims=True)
        for index in range(local_heads)
    ]
    per_group = batch * local_heads // groups
    batches = batch // groups
    place_of = [(row // local_heads, row % local_heads) for row in range(per_group)]
    tile_lane = iota((per_group, LANES), 1)
    tile_row = iota((per_group, LANES), 0)
    column = iota((HEAD_LANES, LANES), 1)
    columns = jnp.zeros((HEAD_LANES, LANES), F32)
    stats = jnp.zeros((per_group, LANES), F32)
    scale = float(HEAD_LANES) ** (-0.5)

    def weigh(group):
        base = group * batches
        rows = jnp.concatenate([query[base + b : base + b + 1] for b, _ in place_of], axis=0)
        wide = [
            jnp.where((tile_lane + low) // HEAD_LANES == tile_row, rows, 0.0)
            for low in range(0, depth, LANES)
        ]
        fade = jnp.concatenate([forgets[h][base + b : base + b + 1] for b, h in place_of], axis=0)
        wide = jnp.concatenate(wide, axis=1).astype(BF16)
        scores = dot(wide, keys[group]) * scale + fade
        scores = scores + decay[base : base + batches].reshape(per_group, -1)
        top = jnp.max(scores, axis=1, keepdims=True)
        short = jnp.exp(scores - top).astype(BF16).astype(F32)
        return top, short, jnp.sum(short, axis=1, keepdims=True)

    ahead = [weigh(group) for group in range(AHEAD)]
    for group in range(groups):
        base = group * batches
        if group + AHEAD < groups:
            ahead.append(weigh(group + AHEAD))
        top, short, total = ahead[group]
        for row in range(per_group):
            wide = jnp.broadcast_to(short[row : row + 1], (8, short.shape[1]))
            spread[group, row] = wide.astype(BF16)
        for row, (b, h) in enumerate(place_of):
            pieces = []
            for first in range(row * HEAD_LANES, (row + 1) * HEAD_LANES, 8):
                mixed = jnp.zeros((8, WIDE), F32)
                for place in range(0, short.shape[1], WIDE):
                    value = values[group, first : first + 8, place : place + WIDE]
                    weight = spread[group, row, :, place : place + WIDE]
                    mixed = mixed + value.astype(F32) * weight.astype(F32)
                pieces.append(mixed[:, :LANES] + mixed[:, LANES:])
            mixed = jnp.concatenate(pieces, axis=0)
            summed = jnp.sum(mixed, axis=1, keepdims=True)
            columns = jnp.where(column == h * batch + base + b, summed, columns)
        stats = jnp.where(tile_lane == group, top, stats)
        stats = jnp.where(tile_lane == HEAD_LANES + group, total, stats)
    flat = jnp.concatenate([columns, columns], axis=0).T
    lane = iota((batch, LANES), 1)
    part[:batch, :] = jnp.where(lane < HEAD_LANES, flat[:batch], flat[batch : 2 * batch])
    part[batch:, :] = stats


def newest_kernel(normed, queries, key_weight, value_weight, newest, own):
    rounded = normed[...]
    key_new = dot(rounded, key_weight[...]).astype(BF16)
    newest[...] = dot(rounded, value_weight[...]).astype(BF16).astype(F32)
    product = queries[...].astype(F32) * key_new.astype(F32)
    low = iota(product.shape, 1) < HEAD_LANES
    scale = float(HEAD_LANES) ** (-0.5)
    one = jnp.sum(jnp.where(low, product, 0.0), axis=1, keepdims=True)
    two = jnp.sum(jnp.where(low, 0.0, product), axis=1, keepdims=True)
    own[...] = jnp.where(low, one, two) * scale


def merge_kernel(local_heads, groups, count, *refs):
    newest, owns, out_weight, short, full = refs[count:]
    batch = newest.shape[0]
    batches = batch // groups
    lane = iota((batch, LANES), 1)
    row = iota((batch, LANES), 0)
    low = lane < HEAD_LANES

    def spread(stats, offset):
        found = []
        for head in range(local_heads):
            picked = stats[head : head + 1]
            for b in range(1, batches):
                index = b * local_heads + head
                picked = jnp.where(row % batches == b, stats[index : index + 1], picked)
            picked = jnp.where(lane == offset + row // batches, picked, 0.0)
            found.append(jnp.sum(picked, axis=1, keepdims=True))
        return jnp.where(low, found[0], found[1])

    tops = [spread(ref[batch:, :], 0) for ref in refs[:count]]
    totals = [spread(ref[batch:, :], HEAD_LANES) for ref in refs[:count]]
    own = owns[...]
    peak = own
    for top in tops:
        peak = jnp.maximum(peak, top)
    own_factor = jnp.exp(own - peak)
    numer = newest[...] * own_factor
    denom = own_factor
    for ref, top, total in zip(refs, tops, totals):
        factor = jnp.exp(top - peak)
        numer = numer + ref[:batch, :] * factor
        denom = denom + total * factor
    product = dot((numer / denom).astype(BF16), out_weight[...])
    full[...] = product
    short[...] = product.astype(BF16)


def add_kernel(*refs):
    total = refs[0][...]
    for ref in refs[1:-1]:
        total = total + ref[...].astype(F32)
    refs[-1][...] = total


def up_kernel(kv, tp, one, two, blocks, gain, up_weight, short, full, piece, middle, mixed):
    first = lax.axis_index("kv") * tp
    total = one[...] + two[...]
    batch = total.shape[0]
    squares = jnp.zeros((batch, LANES), F32)
    for block in range(tp):
        low = block * LANES
        value = (blocks[first + block].astype(F32) + total[:, low : low + LANES]).astype(BF16)
        wide = value.astype(F32)
        middle[block] = wide
        squares = squares + wide * wide
        mixed[:, low : low + LANES] = (wide * gain[pl.ds(first + block, 1), :]).astype(BF16)
    piece[...] = middle[lax.axis_index("tp")]
    product = dot(mixed[...], up_weight[...])
    width = product.shape[1]
    full[...] = product
    for block in range(width // LANES):
        short[block * batch : (block + 1) * batch, :] = product[
            :, block * LANES : (block + 1) * LANES
        ].astype(BF16)
    rest = jnp.sum(squares, axis=1, keepdims=True)
    lane = iota((batch, LANES), 1)
    rest = jnp.where(lane == iota((batch, LANES), 0), rest, 0.0)
    rest = jnp.sum(rest, axis=0, keepdims=True)
    row = iota((PACK, LANES), 0)
    tail = jnp.zeros((PACK, LANES), F32)
    for index in range(3):
        digit = rest.astype(BF16).astype(F32)
        tail = jnp.where(row == index, digit, tail)
        rest = rest - digit
    short[short.shape[0] - PACK :, :] = tail.astype(BF16)


def down_columns(tp, core, active, down_weight, out):
    def columns(pair):
        low = pl.multiple_of((2 * pair + core) * LANES, LANES)
        return down_weight[:, pl.ds(low, LANES)]

    step = 2 if tp % 4 == 0 else 1
    for pair in range(0, tp // 2, step):
        weight = jnp.concatenate([columns(pair + index) for index in range(step)], axis=1)
        product = dot(active, weight)
        for index in range(step):
            out[pair + index] = product[:, index * LANES : (index + 1) * LANES]


def down_kernel(tp, size, count, *refs):
    full, short = refs[0], refs[1]
    others = refs[2 : 1 + count]
    down_weight, hidden, send = refs[1 + count :]
    batch, width = full.shape
    height = width // LANES * batch
    tail = short[height:, :].astype(F32)
    for ref in others:
        tail = tail + ref[height:, :].astype(F32)
    tail = jnp.sum(tail, axis=0, keepdims=True)
    lane = iota((batch, LANES), 1)
    tail = jnp.where(lane == iota((batch, LANES), 0), tail, 0.0)
    inverse = lax.rsqrt(jnp.sum(tail, axis=1, keepdims=True) / size + EPS)
    pieces = []
    for block in range(width // LANES):
        total = full[:, block * LANES : (block + 1) * LANES]
        for ref in others:
            total = total + ref[block * batch : (block + 1) * batch, :].astype(F32)
        active = jnp.maximum(total * inverse, 0.0)
        pieces.append((active * active).astype(BF16))
    active = jnp.concatenate(pieces, axis=1)
    hidden[...] = active
    down_columns(tp, 1 - lax.rem(lax.axis_index("tp"), 2), active, down_weight, send)


def keep_kernel(tp, hidden, down_weight, keep):
    down_columns(tp, lax.rem(lax.axis_index("tp"), 2), hidden[...], down_weight, keep)


def split_kernel(pairs, keep, other, *refs):
    outs, own, shares = refs[:-2], refs[-2], refs[-1]
    shares[...] = keep[...] + other[...]
    place = lax.div(lax.axis_index("tp"), 2)
    own[...] = shares[place]
    for step in range(1, pairs):
        outs[step - 1][...] = shares[lax.rem(place + step, pairs)].astype(BF16)


def last_kernel(*refs):
    total = refs[0][...]
    for ref in refs[1:-1]:
        total = total + ref[...].astype(F32)
    refs[-1][...] = total.astype(BF16)


def shards(
    kv,
    tp,
    stream,
    mixer_gain,
    query_weight,
    key_weight,
    value_weight,
    forget_weight,
    forget_bias,
    key_cache,
    value_cache,
    past_decay,
    out_weight,
    channel_gain,
    up_weight,
    down_weight,
):
    batch, piece_width = stream.shape
    _, local_heads, places, head_size = key_cache.shape
    rows = batch * local_heads
    fits = (
        piece_width == LANES
        and head_size == HEAD_LANES
        and local_heads == LANES // HEAD_LANES
        and tp % 2 == 0
        and kv & (kv - 1) == 0
        and rows == HEAD_LANES
        and batch % PACK == 0
        and up_weight.shape[1] % LANES == 0
        and places % LANES == 0
        and out_weight.shape[1] == tp * LANES
    )
    if not fits:
        return shards_general(
            stream,
            mixer_gain,
            query_weight,
            key_weight,
            value_weight,
            forget_weight,
            forget_bias,
            key_cache,
            value_cache,
            past_decay,
            out_weight,
            channel_gain,
            up_weight,
            down_weight,
        )
    count = kv * tp
    size = count * piece_width
    groups = rows // 8
    depth = 8 * head_size
    (fanned,) = kernel_call(
        fan_kernel,
        [shape_of((count, batch, piece_width), BF16)],
        (stream,),
    )
    (fanned,) = kernel_call(
        hold_kernel,
        [shape_of((count, batch, piece_width), BF16)],
        (fanned,),
        cost=pl.CostEstimate(flops=40_000_000_000, bytes_accessed=0, transcendentals=0),
        aliases={0: 0},
    )
    blocks = lax.all_to_all(fanned, ("kv", "tp"), 0, 0)
    keys = jnp.swapaxes(key_cache, 2, 3).reshape(groups, depth, places)
    values = jnp.swapaxes(value_cache, 2, 3).reshape(groups, depth, places)
    heads = forget_bias.shape[0]
    part, normed, queries = kernel_call(
        functools.partial(attention_kernel, local_heads),
        [
            shape_of((batch + 8, LANES), F32),
            shape_of((batch, size), BF16),
            shape_of((batch, LANES), BF16),
        ],
        (
            blocks,
            mixer_gain.reshape(count, LANES),
            query_weight,
            forget_weight.T,
            forget_bias.reshape(1, heads),
            keys,
            values,
            past_decay,
        ),
        scratch=[pltpu.VMEM((groups, 8, 8, places), BF16)],
    )
    newest, owns = kernel_call(
        newest_kernel,
        [shape_of((batch, LANES), F32)] * 2,
        (normed, queries, key_weight, value_weight),
    )
    def trade(array, step):
        return lax.ppermute(array, "kv", [(i, i ^ step) for i in range(kv)])

    def turn(array, step):
        return lax.ppermute(array, "tp", [(i, (i + 2 * step) % tp) for i in range(tp)])

    def swap(array):
        return lax.ppermute(array, "tp", [(i, i ^ 1) for i in range(tp)])

    pairs = tp // 2
    others = [trade(part, step) for step in range(1, kv)]
    block_width = out_weight.shape[1]
    short, full = kernel_call(
        functools.partial(merge_kernel, local_heads, groups, kv),
        [shape_of((batch, block_width), BF16), shape_of((batch, block_width), F32)],
        (part, *others, newest, owns, out_weight),
    )
    others = [turn(short, step) for step in range(1, pairs)]
    (column_sum,) = kernel_call(add_kernel, [shape_of((batch, block_width), F32)], (full, *others))
    width = up_weight.shape[1]
    short, full, piece = kernel_call(
        functools.partial(up_kernel, kv, tp),
        [
            shape_of((batch * width // LANES + PACK, LANES), BF16),
            shape_of((batch, width), F32),
            shape_of((batch, LANES), F32),
        ],
        (column_sum, swap(column_sum), blocks, channel_gain.reshape(count, LANES), up_weight),
        scratch=[pltpu.VMEM((tp, batch, LANES), F32), pltpu.VMEM((batch, block_width), BF16)],
    )
    others = [trade(short, step) for step in range(1, kv)]
    hidden, send = kernel_call(
        functools.partial(down_kernel, tp, size, kv),
        [shape_of((batch, width), BF16), shape_of((pairs, batch, LANES), F32)],
        (full, short, *others, down_weight),
    )
    (keep,) = kernel_call(
        functools.partial(keep_kernel, tp),
        [shape_of((pairs, batch, LANES), F32)],
        (hidden, down_weight),
    )
    *shares, own = kernel_call(
        functools.partial(split_kernel, pairs),
        [shape_of((batch, LANES), BF16)] * (pairs - 1) + [shape_of((batch, LANES), F32)],
        (keep, swap(send)),
        scratch=[pltpu.VMEM((pairs, batch, LANES), F32)],
    )
    others = [turn(shares[step - 1], step) for step in range(1, pairs)]
    (updated,) = kernel_call(
        last_kernel, [shape_of((batch, LANES), BF16)], (piece, own, *others)
    )
    return updated


def solution(mesh):
    return jax.shard_map(
        functools.partial(shards, mesh.shape["kv"], mesh.shape["tp"]),
        mesh=mesh,
        in_specs=(
            P(None, ("kv", "tp")),
            P(),
            P(None, "tp"),
            P(None, "tp"),
            P(None, "tp"),
            P(),
            P(),
            P(None, "tp", "kv", None),
            P(None, "tp", "kv", None),
            P(None, "tp", "kv"),
            P("tp", "kv"),
            P(),
            P("kv", "tp"),
            P("tp", "kv"),
        ),
        out_specs=P(None, ("kv", "tp")),
        check_vma=False,
    )
```

```python
import functools

import jax
import jax.numpy as jnp
from jax import lax
from jax.experimental import pallas as pl
from jax.experimental.pallas import tpu as pltpu
from jax.sharding import PartitionSpec as P

D = 4096


EPS = 1e-06


def combined_all(part, axis, combine):
    gathered = jax.tree.map(lambda a: lax.all_gather(a, axis), part)

    def take(source):
        return jax.tree.map(lambda a: lax.dynamic_index_in_dim(a, source, 0, False), gathered)

    return lax.fori_loop(
        1, lax.axis_size(axis), lambda source, state: combine(state, take(source)), take(0)
    )


def rms_scale(values, gain):
    widened = values.astype(jnp.float32)
    inverse = lax.rsqrt(jnp.mean(widened * widened, axis=-1, keepdims=True) + EPS)
    return (widened * inverse * gain).astype(jnp.bfloat16)


def merge_parts(earlier, later):
    top_one, total_one, sums_one = earlier
    top_two, total_two, sums_two = later
    highest = jnp.maximum(top_one, top_two)
    factor_one = jnp.exp(top_one - highest)
    factor_two = jnp.exp(top_two - highest)
    return (
        highest,
        total_one * factor_one + total_two * factor_two,
        sums_one * factor_one[..., None] + sums_two * factor_two[..., None],
    )


def squared_relu(values):
    return jnp.square(jax.nn.relu(values)).astype(jnp.bfloat16)


def row_squares(values):
    widened = values.astype(jnp.float32)
    return jnp.sum(widened * widened, axis=1)


def shards_general(
    stream,
    mixer_gain,
    query_weight,
    key_weight,
    value_weight,
    forget_weight,
    forget_bias,
    key_cache,
    value_cache,
    past_decay,
    out_weight,
    channel_gain,
    up_weight,
    down_weight,
):
    batch_rows = stream.shape[0]
    local_heads = key_cache.shape[1]
    head_size = key_cache.shape[3]
    scale_factor = float(head_size) ** (-0.5)
    gathered = lax.all_gather(stream, ("kv", "tp"), axis=1, tiled=True)
    normed = rms_scale(gathered, mixer_gain)
    queries = jnp.dot(normed, query_weight, preferred_element_type=jnp.float32).astype(jnp.bfloat16)
    keys_new = jnp.dot(normed, key_weight, preferred_element_type=jnp.float32).astype(jnp.bfloat16)
    values_new = jnp.dot(normed, value_weight, preferred_element_type=jnp.float32).astype(
        jnp.bfloat16
    )
    forget_all = jax.nn.log_sigmoid(
        jnp.dot(normed, forget_weight, preferred_element_type=jnp.float32) + forget_bias
    )
    forget = lax.dynamic_slice_in_dim(
        forget_all, lax.axis_index("tp") * local_heads, local_heads, 1
    )
    query_heads = queries.reshape(batch_rows, local_heads, head_size)
    scores = (
        jnp.einsum("bhd,bhpd->bhp", query_heads, key_cache, preferred_element_type=jnp.float32)
        * scale_factor
        + forget[..., None]
        + past_decay
    )
    highest = jnp.max(scores, axis=-1)
    weights = jnp.exp(scores - highest[..., None]).astype(jnp.bfloat16)
    totals = jnp.sum(weights.astype(jnp.float32), axis=-1)
    sums = jnp.einsum("bhp,bhpd->bhd", weights, value_cache, preferred_element_type=jnp.float32)
    highest, totals, sums = combined_all((highest, totals, sums), "kv", merge_parts)
    key_heads = keys_new.reshape(batch_rows, local_heads, head_size).astype(jnp.float32)
    value_heads = values_new.reshape(batch_rows, local_heads, head_size).astype(jnp.float32)
    own = jnp.sum(query_heads.astype(jnp.float32) * key_heads, axis=-1) * scale_factor
    peak = jnp.maximum(highest, own)
    cache_factor = jnp.exp(highest - peak)
    own_factor = jnp.exp(own - peak)
    numer = sums * cache_factor[..., None] + value_heads * own_factor[..., None]
    denom = totals * cache_factor + own_factor
    attention = (
        (numer / denom[..., None]).astype(jnp.bfloat16).reshape(batch_rows, local_heads * head_size)
    )
    partial_value = jnp.dot(attention, out_weight, preferred_element_type=jnp.float32)
    piece_width = stream.shape[1]
    block_width = partial_value.shape[1]
    block_sum = lax.psum(partial_value, "tp")
    own_block = lax.dynamic_slice_in_dim(
        gathered, lax.axis_index("kv") * block_width, block_width, 1
    )
    middle_block = (own_block.astype(jnp.float32) + block_sum).astype(jnp.bfloat16)
    squares = lax.psum(row_squares(middle_block), "kv")
    middle_piece = lax.dynamic_slice_in_dim(
        middle_block, lax.axis_index("tp") * piece_width, piece_width, 1
    )
    inverse = lax.rsqrt(squares / D + EPS)
    gain_block = lax.dynamic_slice_in_dim(
        channel_gain, lax.axis_index("kv") * block_width, block_width, 0
    )
    mixed_block = (
        middle_block.astype(jnp.float32) * inverse[:, None] * gain_block[None, :]
    ).astype(jnp.bfloat16)
    up_partial = jnp.dot(mixed_block, up_weight, preferred_element_type=jnp.float32)
    hidden = squared_relu(lax.psum(up_partial, "kv"))
    down_partial = jnp.dot(hidden, down_weight, preferred_element_type=jnp.float32)
    reduced = lax.psum_scatter(down_partial, "tp", scatter_dimension=1, tiled=True)
    return (middle_piece.astype(jnp.float32) + reduced).astype(jnp.bfloat16)


LANES = 128
HEAD_LANES = 64
PACK = 16
WIDE = 256
AHEAD = 2
F32 = jnp.float32
BF16 = jnp.bfloat16
CONTRACT_LAST = (((1,), (1,)), ((), ()))


def iota(shape, axis):
    return lax.broadcasted_iota(jnp.int32, shape, axis)


def dot(one, two):
    return jnp.dot(one, two, preferred_element_type=F32)


def kernel_call(body, out_shapes, arguments, scratch=(), limit=8, cost=None, aliases=None):
    return pl.pallas_call(
        body,
        out_shape=tuple(out_shapes),
        in_specs=[pl.BlockSpec(memory_space=pltpu.VMEM)] * len(arguments),
        out_specs=tuple(pl.BlockSpec(memory_space=pltpu.VMEM) for _ in out_shapes),
        scratch_shapes=list(scratch),
        cost_estimate=cost,
        input_output_aliases=aliases or {},
        compiler_params=pltpu.CompilerParams(vmem_limit_bytes=limit << 20),
    )(*arguments)


def shape_of(shape, dtype):
    return jax.ShapeDtypeStruct(shape, dtype)


def fan_kernel(piece, copies):
    value = piece[...]
    for index in range(copies.shape[0]):
        copies[index] = value


def hold_kernel(copies, same):
    same[0] = copies[0]


def attention_kernel(
    local_heads,
    blocks,
    gain,
    query_weight,
    forget_weight,
    forget_bias,
    keys,
    values,
    decay,
    part,
    normed,
    queries,
    spread,
):
    groups, depth, _ = keys.shape
    count, batch, _ = blocks.shape
    squares = jnp.zeros((batch, LANES), F32)
    for block in range(count):
        wide = blocks[block].astype(F32)
        squares = squares + wide * wide
    mean = jnp.sum(squares, axis=1, keepdims=True) / (count * LANES)
    inverse = lax.rsqrt(mean + EPS)
    for block in range(count):
        scaled = blocks[block].astype(F32) * inverse * gain[block : block + 1, :]
        normed[:, block * LANES : (block + 1) * LANES] = scaled.astype(BF16)
    rounded = normed[...]
    query = dot(rounded, query_weight[...]).astype(BF16)
    queries[...] = query
    query = query.astype(F32)
    logits = lax.dot_general(
        rounded, forget_weight[...], CONTRACT_LAST, preferred_element_type=F32
    )
    logits = logits + forget_bias[...]
    forget = jnp.minimum(logits, 0.0) - jnp.log1p(jnp.exp(-jnp.abs(logits)))
    first_head = lax.axis_index("tp") * local_heads
    head = iota(forget.shape, 1)
    forgets = [
        jnp.sum(jnp.where(head == first_head + index, forget, 0.0), axis=1, keepdims=True)
        for index in range(local_heads)
    ]
    per_group = batch * local_heads // groups
    batches = batch // groups
    place_of = [(row // local_heads, row % local_heads) for row in range(per_group)]
    tile_lane = iota((per_group, LANES), 1)
    tile_row = iota((per_group, LANES), 0)
    column = iota((HEAD_LANES, LANES), 1)
    columns = jnp.zeros((HEAD_LANES, LANES), F32)
    stats = jnp.zeros((per_group, LANES), F32)
    scale = float(HEAD_LANES) ** (-0.5)

    def weigh(group):
        base = group * batches
        rows = jnp.concatenate([query[base + b : base + b + 1] for b, _ in place_of], axis=0)
        wide = [
            jnp.where((tile_lane + low) // HEAD_LANES == tile_row, rows, 0.0)
            for low in range(0, depth, LANES)
        ]
        fade = jnp.concatenate([forgets[h][base + b : base + b + 1] for b, h in place_of], axis=0)
        wide = jnp.concatenate(wide, axis=1).astype(BF16)
        scores = dot(wide, keys[group]) * scale + fade
        scores = scores + decay[base : base + batches].reshape(per_group, -1)
        top = jnp.max(scores, axis=1, keepdims=True)
        short = jnp.exp(scores - top).astype(BF16).astype(F32)
        return top, short, jnp.sum(short, axis=1, keepdims=True)

    ahead = [weigh(group) for group in range(AHEAD)]
    for group in range(groups):
        base = group * batches
        if group + AHEAD < groups:
            ahead.append(weigh(group + AHEAD))
        top, short, total = ahead[group]
        for row in range(per_group):
            wide = jnp.broadcast_to(short[row : row + 1], (8, short.shape[1]))
            spread[group, row] = wide.astype(BF16)
        for row, (b, h) in enumerate(place_of):
            pieces = []
            for first in range(row * HEAD_LANES, (row + 1) * HEAD_LANES, 8):
                mixed = jnp.zeros((8, WIDE), F32)
                for place in range(0, short.shape[1], WIDE):
                    value = values[group, first : first + 8, place : place + WIDE]
                    weight = spread[group, row, :, place : place + WIDE]
                    mixed = mixed + value.astype(F32) * weight.astype(F32)
                pieces.append(mixed[:, :LANES] + mixed[:, LANES:])
            mixed = jnp.concatenate(pieces, axis=0)
            summed = jnp.sum(mixed, axis=1, keepdims=True)
            columns = jnp.where(column == h * batch + base + b, summed, columns)
        stats = jnp.where(tile_lane == group, top, stats)
        stats = jnp.where(tile_lane == HEAD_LANES + group, total, stats)
    flat = jnp.concatenate([columns, columns], axis=0).T
    lane = iota((batch, LANES), 1)
    part[:batch, :] = jnp.where(lane < HEAD_LANES, flat[:batch], flat[batch : 2 * batch])
    part[batch:, :] = stats


def newest_kernel(normed, queries, key_weight, value_weight, newest, own):
    rounded = normed[...]
    key_new = dot(rounded, key_weight[...]).astype(BF16)
    newest[...] = dot(rounded, value_weight[...]).astype(BF16).astype(F32)
    product = queries[...].astype(F32) * key_new.astype(F32)
    low = iota(product.shape, 1) < HEAD_LANES
    scale = float(HEAD_LANES) ** (-0.5)
    one = jnp.sum(jnp.where(low, product, 0.0), axis=1, keepdims=True)
    two = jnp.sum(jnp.where(low, 0.0, product), axis=1, keepdims=True)
    own[...] = jnp.where(low, one, two) * scale


def merge_kernel(local_heads, groups, count, *refs):
    newest, owns, out_weight, short, full = refs[count:]
    batch = newest.shape[0]
    batches = batch // groups
    lane = iota((batch, LANES), 1)
    row = iota((batch, LANES), 0)
    low = lane < HEAD_LANES

    def spread(stats, offset):
        found = []
        for head in range(local_heads):
            picked = stats[head : head + 1]
            for b in range(1, batches):
                index = b * local_heads + head
                picked = jnp.where(row % batches == b, stats[index : index + 1], picked)
            picked = jnp.where(lane == offset + row // batches, picked, 0.0)
            found.append(jnp.sum(picked, axis=1, keepdims=True))
        return jnp.where(low, found[0], found[1])

    tops = [spread(ref[batch:, :], 0) for ref in refs[:count]]
    totals = [spread(ref[batch:, :], HEAD_LANES) for ref in refs[:count]]
    own = owns[...]
    peak = own
    for top in tops:
        peak = jnp.maximum(peak, top)
    own_factor = jnp.exp(own - peak)
    numer = newest[...] * own_factor
    denom = own_factor
    for ref, top, total in zip(refs, tops, totals):
        factor = jnp.exp(top - peak)
        numer = numer + ref[:batch, :] * factor
        denom = denom + total * factor
    product = dot((numer / denom).astype(BF16), out_weight[...])
    full[...] = product
    short[...] = product.astype(BF16)


def add_kernel(*refs):
    total = refs[0][...]
    for ref in refs[1:-1]:
        total = total + ref[...].astype(F32)
    refs[-1][...] = total


def up_kernel(kv, tp, one, two, blocks, gain, up_weight, short, full, piece, middle, mixed):
    first = lax.axis_index("kv") * tp
    total = one[...] + two[...]
    batch = total.shape[0]
    squares = jnp.zeros((batch, LANES), F32)
    for block in range(tp):
        low = block * LANES
        value = (blocks[first + block].astype(F32) + total[:, low : low + LANES]).astype(BF16)
        wide = value.astype(F32)
        middle[block] = wide
        squares = squares + wide * wide
        mixed[:, low : low + LANES] = (wide * gain[pl.ds(first + block, 1), :]).astype(BF16)
    piece[...] = middle[lax.axis_index("tp")]
    product = dot(mixed[...], up_weight[...])
    width = product.shape[1]
    full[...] = product
    for block in range(width // LANES):
        short[block * batch : (block + 1) * batch, :] = product[
            :, block * LANES : (block + 1) * LANES
        ].astype(BF16)
    rest = jnp.sum(squares, axis=1, keepdims=True)
    lane = iota((batch, LANES), 1)
    rest = jnp.where(lane == iota((batch, LANES), 0), rest, 0.0)
    rest = jnp.sum(rest, axis=0, keepdims=True)
    row = iota((PACK, LANES), 0)
    tail = jnp.zeros((PACK, LANES), F32)
    for index in range(3):
        digit = rest.astype(BF16).astype(F32)
        tail = jnp.where(row == index, digit, tail)
        rest = rest - digit
    short[short.shape[0] - PACK :, :] = tail.astype(BF16)


def down_columns(tp, core, active, down_weight, out):
    def columns(pair):
        low = pl.multiple_of((2 * pair + core) * LANES, LANES)
        return down_weight[:, pl.ds(low, LANES)]

    step = 2 if tp % 4 == 0 else 1
    for pair in range(0, tp // 2, step):
        weight = jnp.concatenate([columns(pair + index) for index in range(step)], axis=1)
        product = dot(active, weight)
        for index in range(step):
            out[pair + index] = product[:, index * LANES : (index + 1) * LANES]


def down_kernel(tp, size, count, *refs):
    full, short = refs[0], refs[1]
    others = refs[2 : 1 + count]
    down_weight, hidden, send = refs[1 + count :]
    batch, width = full.shape
    height = width // LANES * batch
    tail = short[height:, :].astype(F32)
    for ref in others:
        tail = tail + ref[height:, :].astype(F32)
    tail = jnp.sum(tail, axis=0, keepdims=True)
    lane = iota((batch, LANES), 1)
    tail = jnp.where(lane == iota((batch, LANES), 0), tail, 0.0)
    inverse = lax.rsqrt(jnp.sum(tail, axis=1, keepdims=True) / size + EPS)
    pieces = []
    for block in range(width // LANES):
        total = full[:, block * LANES : (block + 1) * LANES]
        for ref in others:
            total = total + ref[block * batch : (block + 1) * batch, :].astype(F32)
        active = jnp.maximum(total * inverse, 0.0)
        pieces.append((active * active).astype(BF16))
    active = jnp.concatenate(pieces, axis=1)
    hidden[...] = active
    down_columns(tp, 1 - lax.rem(lax.axis_index("tp"), 2), active, down_weight, send)


def keep_kernel(tp, hidden, down_weight, keep):
    down_columns(tp, lax.rem(lax.axis_index("tp"), 2), hidden[...], down_weight, keep)


def split_kernel(pairs, keep, other, *refs):
    outs, own, shares = refs[:-2], refs[-2], refs[-1]
    shares[...] = keep[...] + other[...]
    place = lax.div(lax.axis_index("tp"), 2)
    own[...] = shares[place]
    for step in range(1, pairs):
        outs[step - 1][...] = shares[lax.rem(place + step, pairs)].astype(BF16)


def last_kernel(*refs):
    total = refs[0][...]
    for ref in refs[1:-1]:
        total = total + ref[...].astype(F32)
    refs[-1][...] = total.astype(BF16)


def shards(
    kv,
    tp,
    stream,
    mixer_gain,
    query_weight,
    key_weight,
    value_weight,
    forget_weight,
    forget_bias,
    key_cache,
    value_cache,
    past_decay,
    out_weight,
    channel_gain,
    up_weight,
    down_weight,
):
    batch, piece_width = stream.shape
    _, local_heads, places, head_size = key_cache.shape
    rows = batch * local_heads
    fits = (
        piece_width == LANES
        and head_size == HEAD_LANES
        and local_heads == LANES // HEAD_LANES
        and tp % 2 == 0
        and kv & (kv - 1) == 0
        and rows == HEAD_LANES
        and batch % PACK == 0
        and up_weight.shape[1] % LANES == 0
        and places % LANES == 0
        and out_weight.shape[1] == tp * LANES
    )
    if not fits:
        return shards_general(
            stream,
            mixer_gain,
            query_weight,
            key_weight,
            value_weight,
            forget_weight,
            forget_bias,
            key_cache,
            value_cache,
            past_decay,
            out_weight,
            channel_gain,
            up_weight,
            down_weight,
        )
    count = kv * tp
    size = count * piece_width
    groups = rows // 8
    depth = 8 * head_size
    (fanned,) = kernel_call(
        fan_kernel,
        [shape_of((count, batch, piece_width), BF16)],
        (stream,),
    )
    (fanned,) = kernel_call(
        hold_kernel,
        [shape_of((count, batch, piece_width), BF16)],
        (fanned,),
        cost=pl.CostEstimate(flops=40_000_000_000, bytes_accessed=0, transcendentals=0),
        aliases={0: 0},
    )
    blocks = lax.all_to_all(fanned, ("kv", "tp"), 0, 0)
    keys = jnp.swapaxes(key_cache, 2, 3).reshape(groups, depth, places)
    values = jnp.swapaxes(value_cache, 2, 3).reshape(groups, depth, places)
    heads = forget_bias.shape[0]
    part, normed, queries = kernel_call(
        functools.partial(attention_kernel, local_heads),
        [
            shape_of((batch + 8, LANES), F32),
            shape_of((batch, size), BF16),
            shape_of((batch, LANES), BF16),
        ],
        (
            blocks,
            mixer_gain.reshape(count, LANES),
            query_weight,
            forget_weight.T,
            forget_bias.reshape(1, heads),
            keys,
            values,
            past_decay,
        ),
        scratch=[pltpu.VMEM((groups, 8, 8, places), BF16)],
    )
    newest, owns = kernel_call(
        newest_kernel,
        [shape_of((batch, LANES), F32)] * 2,
        (normed, queries, key_weight, value_weight),
    )
    def trade(array, step):
        return lax.ppermute(array, "kv", [(i, i ^ step) for i in range(kv)])

    def turn(array, step):
        return lax.ppermute(array, "tp", [(i, (i + 2 * step) % tp) for i in range(tp)])

    def swap(array):
        return lax.ppermute(array, "tp", [(i, i ^ 1) for i in range(tp)])

    pairs = tp // 2
    others = [trade(part, step) for step in range(1, kv)]
    block_width = out_weight.shape[1]
    short, full = kernel_call(
        functools.partial(merge_kernel, local_heads, groups, kv),
        [shape_of((batch, block_width), BF16), shape_of((batch, block_width), F32)],
        (part, *others, newest, owns, out_weight),
    )
    others = [turn(short, step) for step in range(1, pairs)]
    (column_sum,) = kernel_call(add_kernel, [shape_of((batch, block_width), F32)], (full, *others))
    width = up_weight.shape[1]
    short, full, piece = kernel_call(
        functools.partial(up_kernel, kv, tp),
        [
            shape_of((batch * width // LANES + PACK, LANES), BF16),
            shape_of((batch, width), F32),
            shape_of((batch, LANES), F32),
        ],
        (column_sum, swap(column_sum), blocks, channel_gain.reshape(count, LANES), up_weight),
        scratch=[pltpu.VMEM((tp, batch, LANES), F32), pltpu.VMEM((batch, block_width), BF16)],
    )
    others = [trade(short, step) for step in range(1, kv)]
    hidden, send = kernel_call(
        functools.partial(down_kernel, tp, size, kv),
        [shape_of((batch, width), BF16), shape_of((pairs, batch, LANES), F32)],
        (full, short, *others, down_weight),
    )
    (keep,) = kernel_call(
        functools.partial(keep_kernel, tp),
        [shape_of((pairs, batch, LANES), F32)],
        (hidden, down_weight),
    )
    *shares, own = kernel_call(
        functools.partial(split_kernel, pairs),
        [shape_of((batch, LANES), BF16)] * (pairs - 1) + [shape_of((batch, LANES), F32)],
        (keep, swap(send)),
        scratch=[pltpu.VMEM((pairs, batch, LANES), F32)],
    )
    others = [turn(shares[step - 1], step) for step in range(1, pairs)]
    (updated,) = kernel_call(
        last_kernel, [shape_of((batch, LANES), BF16)], (piece, own, *others)
    )
    return updated


def solution(mesh):
    return jax.shard_map(
        functools.partial(shards, mesh.shape["kv"], mesh.shape["tp"]),
        mesh=mesh,
        in_specs=(
            P(None, ("kv", "tp")),
            P(),
            P(None, "tp"),
            P(None, "tp"),
            P(None, "tp"),
            P(),
            P(),
            P(None, "tp", "kv", None),
            P(None, "tp", "kv", None),
            P(None, "tp", "kv"),
            P("tp", "kv"),
            P(),
            P("kv", "tp"),
            P("tp", "kv"),
        ),
        out_specs=P(None, ("kv", "tp")),
        check_vma=False,
    )
```
